32 devices in a mesh: sp: 8 (over z, y), tp: 4 (over x, core).
Axes of the slice: x: 2, y: 2, z: 4, core: 2. Of those that a mesh axis runs over, the one named last changes fastest.
Arguments:
- target: bfloat16 [56, 2048], P('sp'), may hold values from -6 to 6
- source: bfloat16 [2048, 2048], P('sp'), may hold values from -6 to 6
- tgt_gain: float32 [2, 2048], replicated, may hold values from 0.1 to 1.9
- src_gain: float32 [2, 2048], replicated, may hold values from 0.1 to 1.9
- w_query: bfloat16 [2, 2048, 2048], P(None, None, 'tp'), may hold values from -0.125 to 0.125
- w_key: bfloat16 [2, 2048, 2048], P(None, None, 'tp'), may hold values from -0.125 to 0.125
- w_value: bfloat16 [2, 2048, 2048], P(None, None, 'tp'), may hold values from -0.125 to 0.125
- w_out: bfloat16 [2, 2048, 2048], P(None, 'tp'), may hold values from -0.125 to 0.125
- score_scale: float32 [2, 8], P(None, 'tp'), may hold values from 1.5 to 4
Outputs:
- result: bfloat16 [56, 2048], P('sp')
The draws below stay inside these ranges and needn't reach their ends.
All inputs are finite; a program needn't handle non-finite values.
Results may differ from the reference program's by a relative error of at most 0.015.
Values may be sent and summed in bfloat16 or wider, within the bound.
A program may use at most 64 MiB of HBM per device.

```python
import math
import jax
import jax.numpy as jnp
from jax import lax

D = 2048
HEADS = 8
HEAD_DIM = 256
LAYERS = 2
SOURCE = 2048
TOKENS = 56
N_TP = 4


def level_of(rng, shape, cuts, least, top_value):
    factor_of, own = 1.0, jax.random.fold_in(rng, 6)
    for dim, parts in cuts:
        draws = jnp.exp(jax.random.uniform(jax.random.fold_in(own, dim), (parts,), jnp.float32, least / len(cuts), top_value / len(cuts)))
        factor_of = factor_of * jnp.repeat(draws, shape[dim] // parts).reshape([-1 if axis == dim else 1 for axis in range(len(shape))])
    return factor_of


def noise(stream_key, shape, deviation, reach, split=(), kind=jnp.bfloat16):
    array = jax.random.normal(stream_key, shape, jnp.float32) * deviation
    if len(split) > 0:
        array = level_of(stream_key, shape, split, -0.22, 0.18) * array
    return jnp.clip(array, min=-reach, max=reach).astype(kind)


def setup_inputs(seed: int = 0) -> dict:
    arg_keys = jax.random.split(jax.random.key(seed), 10)
    target = noise(arg_keys[0], (TOKENS, D), 1.0, 6.0, ((0, 8),))
    source = noise(arg_keys[1], (SOURCE, D), 1.0, 6.0, ((0, 8),))
    tgt_gain = jnp.clip(1.0 + 0.18 * jax.random.normal(arg_keys[2], (LAYERS, D), jnp.float32), 0.1, 1.9)
    src_gain = jnp.clip(1.0 + 0.18 * jax.random.normal(arg_keys[3], (LAYERS, D), jnp.float32), 0.1, 1.9)
    w_query = noise(arg_keys[4], (LAYERS, D, HEADS * HEAD_DIM), D ** -0.5, 0.125, ((2, 4),))
    w_key = noise(arg_keys[5], (LAYERS, D, HEADS * HEAD_DIM), D ** -0.5, 0.125, ((2, 4),))
    w_value = noise(arg_keys[6], (LAYERS, D, HEADS * HEAD_DIM), D ** -0.5, 0.125, ((2, 4),))
    w_out = noise(arg_keys[7], (LAYERS, HEADS * HEAD_DIM, D), (HEADS * HEAD_DIM) ** -0.5, 0.125, ((1, 4),))
    score_scale = jnp.clip(jnp.exp(math.log(4.0) - 0.98082925 * jax.random.uniform(arg_keys[8], (LAYERS, HEADS), jnp.float32) ** level_of(arg_keys[8], (LAYERS, HEADS), ((1, 4),), -0.2, 0.2)), 1.5, 4.0)
    return {"target": target, "source": source, "tgt_gain": tgt_gain, "src_gain": src_gain, "w_query": w_query, "w_key": w_key, "w_value": w_value, "w_out": w_out, "score_scale": score_scale}


EPS = 1e-06

def row_scale(values):
    return lax.rsqrt(lax.optimization_barrier(jnp.mean(values * values, axis=-1, keepdims=True)) + EPS)

def head_norm(projected):
    heads = projected.reshape(projected.shape[0], -1, HEAD_DIM)
    heads = heads * row_scale(heads)
    return heads.reshape(projected.shape).astype(jnp.bfloat16)

def reference(target, source, tgt_gain, src_gain, w_query, w_key, w_value, w_out, score_scale):
    root = math.sqrt(HEAD_DIM)
    src_float = source.astype(jnp.float32)
    src_scale = row_scale(src_float)
    hidden = target
    group_heads = HEADS // N_TP
    for layer_index in range(LAYERS):
        normed_src = (src_float * src_scale * src_gain[layer_index]).astype(jnp.bfloat16)
        keys = head_norm(jnp.dot(normed_src, w_key[layer_index], preferred_element_type=jnp.float32))
        values = jnp.dot(normed_src, w_value[layer_index], preferred_element_type=jnp.float32).astype(jnp.bfloat16)
        hidden_float = hidden.astype(jnp.float32)
        normed_tgt = (hidden_float * row_scale(hidden_float) * tgt_gain[layer_index]).astype(jnp.bfloat16)
        queries = head_norm(jnp.dot(normed_tgt, w_query[layer_index], preferred_element_type=jnp.float32))
        query_heads = queries.reshape(TOKENS, HEADS, HEAD_DIM).transpose(1, 0, 2)
        key_heads = keys.reshape(SOURCE, HEADS, HEAD_DIM).transpose(1, 0, 2)
        value_heads = values.reshape(SOURCE, HEADS, HEAD_DIM).transpose(1, 0, 2)

        def one_head(inputs):
            query_one, key_one, value_one, scale_one = inputs
            scores = jnp.dot(query_one, key_one.T, preferred_element_type=jnp.float32)
            logits = scale_one * (scores / root - root)
            weights = jnp.exp(logits)
            denominators = lax.optimization_barrier(jnp.sum(weights, axis=1))
            numerators = jnp.dot(weights.astype(jnp.bfloat16), value_one, preferred_element_type=jnp.float32)
            return (numerators / denominators[:, None]).astype(jnp.bfloat16)
        outputs = lax.map(one_head, (query_heads, key_heads, value_heads, score_scale[layer_index]))
        attended = outputs.transpose(1, 0, 2).reshape(TOKENS, HEADS * HEAD_DIM)
        branch = jnp.zeros((TOKENS, D), jnp.float32)
        group_width = group_heads * HEAD_DIM
        for group in range(N_TP):
            columns = attended[:, group * group_width:(group + 1) * group_width]
            rows_out = w_out[layer_index, group * group_width:(group + 1) * group_width, :]
            share = jnp.dot(columns, rows_out, preferred_element_type=jnp.float32).astype(jnp.bfloat16)
            branch = branch + share.astype(jnp.float32)
        hidden = (hidden_float + branch).astype(jnp.bfloat16)
    return hidden
```

```python
import functools
import math

import jax
import jax.numpy as jnp
from jax import lax
from jax.experimental import pallas as pl
from jax.experimental.pallas import tpu as pltpu
from jax.sharding import PartitionSpec as P

HEAD_DIM = 256
EPS = 1e-06
LANES = 128
SUBLANES = 8
MESH = pl.DeviceIdType.MESH
BF16 = jnp.bfloat16
F32 = jnp.float32


def row_scale(values):
    return lax.rsqrt(jnp.mean(values * values, axis=-1, keepdims=True) + EPS)


def each(count, step):
    if count <= 8:
        for index in range(count):
            step(index)
    else:

        def turn(index, carry):
            step(index)
            return carry

        lax.fori_loop(0, count, turn, 0)


def kernel(
    n_sp,
    n_tp,
    target,
    source,
    tgt_gain,
    src_gain,
    w_query,
    w_key,
    w_value,
    w_out,
    score_scale,
    out,
    tgt_v,
    src_v,
    tg_v,
    sg_v,
    wq_v,
    wk_v,
    wv_v,
    wo_v,
    scale_s,
    out_v,
    hid,
    normed,
    keys,
    vals,
    q_all,
    num_send,
    num_recv,
    shares,
    load_sem,
    w_sem,
    send_sem,
    recv_sem,
):
    layers = w_query.shape[0]
    rows = target.shape[0]
    pad = hid.shape[0]
    width = w_query.shape[2]
    heads = width // HEAD_DIM
    src_rows = source.shape[0]
    root = math.sqrt(HEAD_DIM)
    me_s = lax.axis_index("sp")
    me_t = lax.axis_index("tp")

    def sp_peer(step):
        return lax.rem(me_s + step + 1, n_sp)

    def tp_peer(step):
        return lax.rem(me_t + step + 1, n_tp)

    small = [
        pltpu.make_async_copy(target, tgt_v, load_sem.at[0]),
        pltpu.make_async_copy(tgt_gain, tg_v, load_sem.at[1]),
        pltpu.make_async_copy(src_gain, sg_v, load_sem.at[2]),
        pltpu.make_async_copy(score_scale, scale_s, load_sem.at[3]),
        pltpu.make_async_copy(source, src_v, load_sem.at[4]),
    ]
    big = {}
    for layer in range(layers):
        for kind, (hbm, vmem) in enumerate(
            ((w_query, wq_v), (w_key, wk_v), (w_value, wv_v), (w_out, wo_v))
        ):
            big[layer, kind] = pltpu.make_async_copy(
                hbm.at[layer], vmem.at[layer], w_sem.at[layer, kind]
            )
    for copy in small:
        copy.start()
    big[0, 0].start()
    big[0, 1].start()
    big[0, 2].start()

    barrier = pltpu.get_barrier_semaphore()

    def greet_sp(step):
        pl.semaphore_signal(
            barrier, inc=1, device_id={"sp": sp_peer(step)}, device_id_type=MESH
        )

    def greet_tp(step):
        pl.semaphore_signal(
            barrier, inc=1, device_id={"tp": tp_peer(step)}, device_id_type=MESH
        )

    each(n_sp - 1, greet_sp)
    each(n_tp - 1, greet_tp)

    def remote(src, dst, stage, layer, target_id):
        return pltpu.make_async_remote_copy(
            src_ref=src,
            dst_ref=dst,
            send_sem=send_sem.at[layer, stage],
            recv_sem=recv_sem.at[layer, stage],
            device_id=target_id,
            device_id_type=MESH,
        )

    def wait_bytes(ref, sem):
        pltpu.make_async_copy(ref, ref, sem).wait()

    def head_norm(block):
        return (block * row_scale(block)).astype(BF16)

    def make_queries(layer):
        hidden = hid[...]
        normed_tgt = (hidden * row_scale(hidden) * tg_v[layer : layer + 1, :]).astype(BF16)
        for head in range(heads):
            cols = slice(head * HEAD_DIM, (head + 1) * HEAD_DIM)
            block = jnp.dot(normed_tgt, wq_v[layer, :, cols], preferred_element_type=F32)
            q_all[layer, me_s, :, cols] = head_norm(block)

    def send_queries(layer):
        def go(step):
            remote(
                q_all.at[layer, me_s], q_all.at[layer, me_s], 0, layer, {"sp": sp_peer(step)}
            ).start()

        each(n_sp - 1, go)

    def make_source(layer):
        rows_in = normed[layer]
        big[layer, 1].wait()
        for head in range(heads):
            cols = slice(head * HEAD_DIM, (head + 1) * HEAD_DIM)
            block = jnp.dot(rows_in, wk_v[layer, :, cols], preferred_element_type=F32)
            keys[layer, head] = head_norm(block)
        big[layer, 2].wait()
        for head in range(heads):
            cols = slice(head * HEAD_DIM, (head + 1) * HEAD_DIM)
            block = jnp.dot(rows_in, wv_v[layer, :, cols], preferred_element_type=F32)
            vals[layer, head] = block.astype(BF16)

    chunk = math.gcd(n_sp, 8)
    count = chunk * pad

    def attend(layer):
        def one(step):
            first = step * chunk
            lane = lax.broadcasted_iota(jnp.int32, (count, LANES), 1)
            extra = jnp.zeros((count, LANES), F32)
            queries = q_all[layer, pl.ds(first, chunk)].astype(F32).reshape(count, width)
            for head in range(heads):
                cols = slice(head * HEAD_DIM, (head + 1) * HEAD_DIM)
                scores = lax.dot_general(
                    queries[:, cols].astype(BF16),
                    keys[layer, head],
                    (((1,), (1,)), ((), ())),
                    preferred_element_type=F32,
                )
                weights = jnp.exp(scale_s[layer, head] * (scores / root - root))
                denom = jnp.sum(weights, axis=1, keepdims=True)
                high = denom.astype(BF16).astype(F32)
                extra = jnp.where(lane == 2 * head, high, extra)
                extra = jnp.where(lane == 2 * head + 1, denom - high, extra)
                numer = jnp.dot(
                    weights.astype(BF16), vals[layer, head], preferred_element_type=F32
                )
                num_send[layer, pl.ds(first, chunk), :, cols] = numer.reshape(
                    chunk, pad, HEAD_DIM
                ).astype(BF16)
            num_send[layer, pl.ds(first, chunk), :, width:] = extra.reshape(
                chunk, pad, LANES
            ).astype(BF16)

        each(n_sp // chunk, one)

    def send_numerators(layer):
        def go(step):
            peer = sp_peer(step)
            remote(
                num_send.at[layer, peer], num_recv.at[layer, me_s], 1, layer, {"sp": peer}
            ).start()

        each(n_sp - 1, go)
        num_recv[layer, me_s] = num_send[layer, me_s]

    def finish_attention(layer):
        wait_bytes(num_recv.at[layer, pl.ds(0, n_sp - 1)], recv_sem.at[layer, 1])
        total = jnp.sum(num_recv[layer].astype(F32), axis=0)
        pieces = []
        for head in range(heads):
            cols = slice(head * HEAD_DIM, (head + 1) * HEAD_DIM)
            at = width + 2 * head
            denom = total[:, at : at + 1] + total[:, at + 1 : at + 2]
            pieces.append((total[:, cols] / denom).astype(BF16))
        return pieces

    def send_shares(layer, pieces):
        acc = None
        for head in range(heads):
            part = jnp.dot(
                pieces[head],
                wo_v[layer, head * HEAD_DIM : (head + 1) * HEAD_DIM, :],
                preferred_element_type=F32,
            )
            acc = part if acc is None else acc + part
        shares[layer, me_t] = acc.astype(BF16)

        def go(step):
            remote(
                shares.at[layer, me_t], shares.at[layer, me_t], 2, layer, {"tp": tp_peer(step)}
            ).start()

        each(n_tp - 1, go)

    small[0].wait()
    small[1].wait()
    hid[...] = jnp.zeros_like(hid)
    hid[0:rows, :] = tgt_v[...].astype(F32)
    big[0, 0].wait()
    make_queries(0)
    for layer in range(layers):
        for kind in (1, 2, 3, 0):
            if (layer, kind) not in ((0, 0), (0, 1), (0, 2)):
                big[layer, kind].start()
    pl.semaphore_wait(barrier, n_sp - 1 + n_tp - 1)
    send_queries(0)

    small[2].wait()
    small[4].wait()
    step_rows = math.gcd(src_rows, 16)

    def norm_rows(index, carry):
        at = pl.ds(pl.multiple_of(index * step_rows, step_rows), step_rows)
        block = src_v[at, :].astype(F32)
        block = block * row_scale(block)
        for layer in range(layers):
            normed[layer, at, :] = (block * sg_v[layer : layer + 1, :]).astype(BF16)
        return carry

    lax.fori_loop(0, src_rows // step_rows, norm_rows, 0)
    small[3].wait()
    for layer in range(layers):
        make_source(layer)

    for layer in range(layers):
        if layer > 0:
            big[layer, 0].wait()
            make_queries(layer)
            send_queries(layer)
        wait_bytes(q_all.at[layer, pl.ds(0, n_sp - 1)], recv_sem.at[layer, 0])
        attend(layer)
        send_numerators(layer)
        big[layer, 3].wait()
        send_shares(layer, finish_attention(layer))
        wait_bytes(shares.at[layer, pl.ds(0, n_tp - 1)], recv_sem.at[layer, 2])
        branch = jnp.sum(shares[layer].astype(F32), axis=0)
        hid[...] = (hid[...] + branch).astype(BF16).astype(F32)

    out_v[...] = hid[0:rows, :].astype(BF16)
    final = pltpu.make_async_copy(out_v, out, load_sem.at[5])
    final.start()
    for layer in range(layers):
        wait_bytes(q_all.at[layer, pl.ds(0, n_sp - 1)], send_sem.at[layer, 0])
        wait_bytes(num_recv.at[layer, pl.ds(0, n_sp - 1)], send_sem.at[layer, 1])
        wait_bytes(shares.at[layer, pl.ds(0, n_tp - 1)], send_sem.at[layer, 2])
    final.wait()


def solution(mesh):
    n_sp, n_tp = mesh.shape["sp"], mesh.shape["tp"]
    placed = (
        P("sp", None),
        P("sp", None),
        P(),
        P(),
        P(None, None, "tp"),
        P(None, None, "tp"),
        P(None, None, "tp"),
        P(None, "tp", None),
        P(None, "tp"),
    )

    def body(*args):
        target, source, tgt_gain, src_gain, w_query, w_key, w_value, w_out, score_scale = args
        layers, model, width = w_query.shape
        rows = target.shape[0]
        src_rows = source.shape[0]
        heads = width // HEAD_DIM
        pad = -(-rows // SUBLANES) * SUBLANES
        anywhere = pl.BlockSpec(memory_space=pl.ANY)
        return pl.pallas_call(
            functools.partial(kernel, n_sp, n_tp),
            out_shape=jax.ShapeDtypeStruct(target.shape, BF16),
            in_specs=[anywhere] * len(args),
            out_specs=anywhere,
            scratch_shapes=[
                pltpu.VMEM(target.shape, BF16),
                pltpu.VMEM(source.shape, BF16),
                pltpu.VMEM(tgt_gain.shape, F32),
                pltpu.VMEM(src_gain.shape, F32),
                pltpu.VMEM(w_query.shape, BF16),
                pltpu.VMEM(w_key.shape, BF16),
                pltpu.VMEM(w_value.shape, BF16),
                pltpu.VMEM(w_out.shape, BF16),
                pltpu.SMEM(score_scale.shape, F32),
                pltpu.VMEM(target.shape, BF16),
                pltpu.VMEM((pad, model), F32),
                pltpu.VMEM((layers, src_rows, model), BF16),
                pltpu.VMEM((layers, heads, src_rows, HEAD_DIM), BF16),
                pltpu.VMEM((layers, heads, src_rows, HEAD_DIM), BF16),
                pltpu.VMEM((layers, n_sp, pad, width), BF16),
                pltpu.VMEM((layers, n_sp, pad, width + LANES), BF16),
                pltpu.VMEM((layers, n_sp, pad, width + LANES), BF16),
                pltpu.VMEM((layers, n_tp, pad, model), BF16),
                pltpu.SemaphoreType.DMA((6,)),
                pltpu.SemaphoreType.DMA((layers, 4)),
                pltpu.SemaphoreType.DMA((layers, 3)),
                pltpu.SemaphoreType.DMA((layers, 3)),
            ],
            compiler_params=pltpu.CompilerParams(
                collective_id=0, has_side_effects=True, vmem_limit_bytes=60 * 1024 * 1024
            ),
        )(*args)

    return jax.shard_map(
        body, mesh=mesh, in_specs=placed, out_specs=P("sp", None), check_vma=False
    )
```

```python
import functools
import math

import jax
import jax.numpy as jnp
from jax import lax
from jax.experimental import pallas as pl
from jax.experimental.pallas import tpu as pltpu
from jax.sharding import PartitionSpec as P

HEAD_DIM = 256
EPS = 1e-06
LANES = 128
SUBLANES = 8
MESH = pl.DeviceIdType.MESH
BF16 = jnp.bfloat16
F32 = jnp.float32


def row_scale(values):
    return lax.rsqrt(jnp.mean(values * values, axis=-1, keepdims=True) + EPS)


def each(count, step):
    if count <= 8:
        for index in range(count):
            step(index)
    else:

        def turn(index, carry):
            step(index)
            return carry

        lax.fori_loop(0, count, turn, 0)


def kernel(
    n_sp,
    n_tp,
    target,
    source,
    tgt_gain,
    src_gain,
    w_query,
    w_key,
    w_value,
    w_out,
    score_scale,
    out,
    tgt_v,
    src_v,
    tg_v,
    sg_v,
    wq_v,
    wk_v,
    wv_v,
    wo_v,
    scale_s,
    out_v,
    hid,
    normed,
    keys,
    vals,
    q_all,
    num_send,
    num_recv,
    shares,
    load_sem,
    w_sem,
    send_sem,
    recv_sem,
):
    layers = w_query.shape[0]
    rows = target.shape[0]
    pad = hid.shape[0]
    width = w_query.shape[2]
    heads = width // HEAD_DIM
    src_rows = source.shape[0]
    root = math.sqrt(HEAD_DIM)
    me_s = lax.axis_index("sp")
    me_t = lax.axis_index("tp")

    def sp_peer(step):
        return lax.rem(me_s + step + 1, n_sp)

    def tp_peer(step):
        return lax.rem(me_t + step + 1, n_tp)

    small = [
        pltpu.make_async_copy(target, tgt_v, load_sem.at[0]),
        pltpu.make_async_copy(tgt_gain, tg_v, load_sem.at[1]),
        pltpu.make_async_copy(src_gain, sg_v, load_sem.at[2]),
        pltpu.make_async_copy(score_scale, scale_s, load_sem.at[3]),
        pltpu.make_async_copy(source, src_v, load_sem.at[4]),
    ]
    big = {}
    for layer in range(layers):
        for kind, (hbm, vmem) in enumerate(
            ((w_query, wq_v), (w_key, wk_v), (w_value, wv_v), (w_out, wo_v))
        ):
            big[layer, kind] = pltpu.make_async_copy(
                hbm.at[layer], vmem.at[layer], w_sem.at[layer, kind]
            )
    for copy in small:
        copy.start()
    big[0, 0].start()
    big[0, 1].start()
    big[0, 2].start()

    barrier = pltpu.get_barrier_semaphore()

    def greet_sp(step):
        pl.semaphore_signal(
            barrier, inc=1, device_id={"sp": sp_peer(step)}, device_id_type=MESH
        )

    def greet_tp(step):
        pl.semaphore_signal(
            barrier, inc=1, device_id={"tp": tp_peer(step)}, device_id_type=MESH
        )

    each(n_sp - 1, greet_sp)
    each(n_tp - 1, greet_tp)

    def remote(src, dst, stage, layer, target_id):
        return pltpu.make_async_remote_copy(
            src_ref=src,
            dst_ref=dst,
            send_sem=send_sem.at[layer, stage],
            recv_sem=recv_sem.at[layer, stage],
            device_id=target_id,
            device_id_type=MESH,
        )

    def wait_bytes(ref, sem):
        pltpu.make_async_copy(ref, ref, sem).wait()

    def head_norm(block):
        return (block * row_scale(block)).astype(BF16)

    def make_queries(layer):
        hidden = hid[...]
        normed_tgt = (hidden * row_scale(hidden) * tg_v[layer : layer + 1, :]).astype(BF16)
        for head in range(heads):
            cols = slice(head * HEAD_DIM, (head + 1) * HEAD_DIM)
            block = jnp.dot(normed_tgt, wq_v[layer, :, cols], preferred_element_type=F32)
            q_all[layer, me_s, :, cols] = head_norm(block)

    def send_queries(layer):
        def go(step):
            remote(
                q_all.at[layer, me_s], q_all.at[layer, me_s], 0, layer, {"sp": sp_peer(step)}
            ).start()

        each(n_sp - 1, go)

    def make_source(layer):
        rows_in = normed[layer]
        big[layer, 1].wait()
        for head in range(heads):
            cols = slice(head * HEAD_DIM, (head + 1) * HEAD_DIM)
            block = jnp.dot(rows_in, wk_v[layer, :, cols], preferred_element_type=F32)
            keys[layer, head] = head_norm(block)
        big[layer, 2].wait()
        for head in range(heads):
            cols = slice(head * HEAD_DIM, (head + 1) * HEAD_DIM)
            block = jnp.dot(rows_in, wv_v[layer, :, cols], preferred_element_type=F32)
            vals[layer, head] = block.astype(BF16)

    chunk = math.gcd(n_sp, 8)
    count = chunk * pad

    def attend(layer):
        def one(step):
            first = step * chunk
            lane = lax.broadcasted_iota(jnp.int32, (count, LANES), 1)
            extra = jnp.zeros((count, LANES), F32)
            queries = q_all[layer, pl.ds(first, chunk)].astype(F32).reshape(count, width)
            for head in range(heads):
                cols = slice(head * HEAD_DIM, (head + 1) * HEAD_DIM)
                scores = lax.dot_general(
                    queries[:, cols].astype(BF16),
                    keys[layer, head],
                    (((1,), (1,)), ((), ())),
                    preferred_element_type=F32,
                )
                weights = jnp.exp(scale_s[layer, head] * (scores / root - root))
                denom = jnp.sum(weights, axis=1, keepdims=True)
                high = denom.astype(BF16).astype(F32)
                extra = jnp.where(lane == 2 * head, high, extra)
                extra = jnp.where(lane == 2 * head + 1, denom - high, extra)
                numer = jnp.dot(
                    weights.astype(BF16), vals[layer, head], preferred_element_type=F32
                )
                num_send[layer, pl.ds(first, chunk), :, cols] = numer.reshape(
                    chunk, pad, HEAD_DIM
                ).astype(BF16)
            num_send[layer, pl.ds(first, chunk), :, width:] = extra.reshape(
                chunk, pad, LANES
            ).astype(BF16)

        each(n_sp // chunk, one)

    def send_numerators(layer):
        def go(step):
            peer = sp_peer(step)
            remote(
                num_send.at[layer, peer], num_recv.at[layer, me_s], 1, layer, {"sp": peer}
            ).start()

        each(n_sp - 1, go)
        num_recv[layer, me_s] = num_send[layer, me_s]

    def finish_attention(layer):
        wait_bytes(num_recv.at[layer, pl.ds(0, n_sp - 1)], recv_sem.at[layer, 1])
        total = jnp.sum(num_recv[layer].astype(F32), axis=0)
        pieces = []
        for head in range(heads):
            cols = slice(head * HEAD_DIM, (head + 1) * HEAD_DIM)
            at = width + 2 * head
            denom = total[:, at : at + 1] + total[:, at + 1 : at + 2]
            pieces.append((total[:, cols] / denom).astype(BF16))
        return pieces

    def send_shares(layer, pieces):
        acc = None
        for head in range(heads):
            part = jnp.dot(
                pieces[head],
                wo_v[layer, head * HEAD_DIM : (head + 1) * HEAD_DIM, :],
                preferred_element_type=F32,
            )
            acc = part if acc is None else acc + part
        shares[layer, me_t] = acc.astype(BF16)

        def go(step):
            remote(
                shares.at[layer, me_t], shares.at[layer, me_t], 2, layer, {"tp": tp_peer(step)}
            ).start()

        each(n_tp - 1, go)

    small[0].wait()
    small[1].wait()
    hid[...] = jnp.zeros_like(hid)
    hid[0:rows, :] = tgt_v[...].astype(F32)
    big[0, 0].wait()
    make_queries(0)
    for layer in range(layers):
        for kind in (1, 2, 3, 0):
            if (layer, kind) not in ((0, 0), (0, 1), (0, 2)):
                big[layer, kind].start()
    pl.semaphore_wait(barrier, n_sp - 1 + n_tp - 1)
    send_queries(0)

    small[2].wait()
    small[4].wait()
    step_rows = math.gcd(src_rows, 16)

    def norm_source(layer):
        def norm_rows(index, carry):
            at = pl.ds(pl.multiple_of(index * step_rows, step_rows), step_rows)
            block = src_v[at, :].astype(F32)
            block = block * row_scale(block) * sg_v[layer : layer + 1, :]
            normed[layer, at, :] = block.astype(BF16)
            return carry

        lax.fori_loop(0, src_rows // step_rows, norm_rows, 0)

    norm_source(0)
    small[3].wait()
    make_source(0)

    for layer in range(layers):
        if layer > 0:
            big[layer, 0].wait()
            make_queries(layer)
            send_queries(layer)
        wait_bytes(q_all.at[layer, pl.ds(0, n_sp - 1)], recv_sem.at[layer, 0])
        attend(layer)
        send_numerators(layer)
        if layer + 1 < layers:
            norm_source(layer + 1)
            make_source(layer + 1)
        big[layer, 3].wait()
        send_shares(layer, finish_attention(layer))
        wait_bytes(shares.at[layer, pl.ds(0, n_tp - 1)], recv_sem.at[layer, 2])
        branch = jnp.sum(shares[layer].astype(F32), axis=0)
        hid[...] = (hid[...] + branch).astype(BF16).astype(F32)

    out_v[...] = hid[0:rows, :].astype(BF16)
    final = pltpu.make_async_copy(out_v, out, load_sem.at[5])
    final.start()
    for layer in range(layers):
        wait_bytes(q_all.at[layer, pl.ds(0, n_sp - 1)], send_sem.at[layer, 0])
        wait_bytes(num_recv.at[layer, pl.ds(0, n_sp - 1)], send_sem.at[layer, 1])
        wait_bytes(shares.at[layer, pl.ds(0, n_tp - 1)], send_sem.at[layer, 2])
    final.wait()


def solution(mesh):
    n_sp, n_tp = mesh.shape["sp"], mesh.shape["tp"]
    placed = (
        P("sp", None),
        P("sp", None),
        P(),
        P(),
        P(None, None, "tp"),
        P(None, None, "tp"),
        P(None, None, "tp"),
        P(None, "tp", None),
        P(None, "tp"),
    )

    def body(*args):
        target, source, tgt_gain, src_gain, w_query, w_key, w_value, w_out, score_scale = args
        layers, model, width = w_query.shape
        rows = target.shape[0]
        src_rows = source.shape[0]
        heads = width // HEAD_DIM
        pad = -(-rows // SUBLANES) * SUBLANES
        anywhere = pl.BlockSpec(memory_space=pl.ANY)
        return pl.pallas_call(
            functools.partial(kernel, n_sp, n_tp),
            out_shape=jax.ShapeDtypeStruct(target.shape, BF16),
            in_specs=[anywhere] * len(args),
            out_specs=anywhere,
            scratch_shapes=[
                pltpu.VMEM(target.shape, BF16),
                pltpu.VMEM(source.shape, BF16),
                pltpu.VMEM(tgt_gain.shape, F32),
                pltpu.VMEM(src_gain.shape, F32),
                pltpu.VMEM(w_query.shape, BF16),
                pltpu.VMEM(w_key.shape, BF16),
                pltpu.VMEM(w_value.shape, BF16),
                pltpu.VMEM(w_out.shape, BF16),
                pltpu.SMEM(score_scale.shape, F32),
                pltpu.VMEM(target.shape, BF16),
                pltpu.VMEM((pad, model), F32),
                pltpu.VMEM((layers, src_rows, model), BF16),
                pltpu.VMEM((layers, heads, src_rows, HEAD_DIM), BF16),
                pltpu.VMEM((layers, heads, src_rows, HEAD_DIM), BF16),
                pltpu.VMEM((layers, n_sp, pad, width), BF16),
                pltpu.VMEM((layers, n_sp, pad, width + LANES), BF16),
                pltpu.VMEM((layers, n_sp, pad, width + LANES), BF16),
                pltpu.VMEM((layers, n_tp, pad, model), BF16),
                pltpu.SemaphoreType.DMA((6,)),
                pltpu.SemaphoreType.DMA((layers, 4)),
                pltpu.SemaphoreType.DMA((layers, 3)),
                pltpu.SemaphoreType.DMA((layers, 3)),
            ],
            compiler_params=pltpu.CompilerParams(
                collective_id=0, has_side_effects=True, vmem_limit_bytes=60 * 1024 * 1024
            ),
        )(*args)

    return jax.shard_map(
        body, mesh=mesh, in_specs=placed, out_specs=P("sp", None), check_vma=False
    )
```

```python
import functools
import math

import jax
import jax.numpy as jnp
from jax import lax
from jax.experimental import pallas as pl
from jax.experimental.pallas import tpu as pltpu
from jax.sharding import PartitionSpec as P

HEAD_DIM = 256
EPS = 1e-06
PARTS = 4
SUBLANES = 8
MESH = pl.DeviceIdType.MESH
BF16 = jnp.bfloat16
F32 = jnp.float32


def row_scale(values):
    return lax.rsqrt(jnp.mean(values * values, axis=-1, keepdims=True) + EPS)


def each(count, step):
    if count <= 8:
        for index in range(count):
            step(index)
    else:

        def turn(index, carry):
            step(index)
            return carry

        lax.fori_loop(0, count, turn, 0)


def kernel(
    n_sp,
    n_tp,
    target,
    source,
    tgt_gain,
    src_gain,
    w_query,
    w_key,
    w_value,
    w_out,
    score_scale,
    out,
    tgt_v,
    src_v,
    tg_v,
    sg_v,
    wq_v,
    wk_v,
    wv_v,
    wo_v,
    scale_s,
    out_v,
    hid,
    normed,
    keys,
    vals,
    q_all,
    num_send,
    num_recv,
    shares,
    load_sem,
    w_sem,
    *sems,
):
    q_sems, n_sems, s_sems = sems[0:2], sems[2:4], sems[4:6]
    parts, part_width = shares.shape[1], shares.shape[4]
    layers = w_query.shape[0]
    rows = target.shape[0]
    pad = hid.shape[0]
    width = w_query.shape[2]
    heads = width // HEAD_DIM
    src_rows = source.shape[0]
    root = math.sqrt(HEAD_DIM)
    me_s = lax.axis_index("sp")
    me_t = lax.axis_index("tp")

    def peer_of(me, step, size):
        if size & (size - 1):
            return lax.rem(me + step + 1, size)
        distance = size - 1 - step
        peer = me
        bit = 1
        while bit < size:
            here = lax.rem(me // bit, 2)
            flip = (distance // bit) % 2
            peer = peer + flip * bit * (1 - 2 * here)
            bit *= 2
        return peer

    def sp_peer(step):
        return peer_of(me_s, step, n_sp)

    def tp_peer(step):
        return peer_of(me_t, step, n_tp)

    small = [
        pltpu.make_async_copy(target, tgt_v, load_sem.at[0]),
        pltpu.make_async_copy(tgt_gain, tg_v, load_sem.at[1]),
        pltpu.make_async_copy(src_gain, sg_v, load_sem.at[2]),
        pltpu.make_async_copy(score_scale, scale_s, load_sem.at[3]),
        pltpu.make_async_copy(source, src_v, load_sem.at[4]),
    ]
    big = {}
    for layer in range(layers):
        for kind, (hbm, vmem) in enumerate(
            ((w_query, wq_v), (w_key, wk_v), (w_value, wv_v), (w_out, wo_v))
        ):
            big[layer, kind] = pltpu.make_async_copy(
                hbm.at[layer], vmem.at[layer], w_sem.at[layer, kind]
            )
    for copy in small:
        copy.start()
    big[0, 0].start()
    big[0, 1].start()
    big[0, 2].start()

    barrier = pltpu.get_barrier_semaphore()

    def greet_sp(step):
        pl.semaphore_signal(
            barrier, inc=1, device_id={"sp": sp_peer(step)}, device_id_type=MESH
        )

    def greet_tp(step):
        pl.semaphore_signal(
            barrier, inc=1, device_id={"tp": tp_peer(step)}, device_id_type=MESH
        )

    each(n_sp - 1, greet_sp)
    each(n_tp - 1, greet_tp)

    def remote(src, dst, sems, at, target_id):
        return pltpu.make_async_remote_copy(
            src_ref=src,
            dst_ref=dst,
            send_sem=sems[0].at[at],
            recv_sem=sems[1].at[at],
            device_id=target_id,
            device_id_type=MESH,
        )

    def wait_bytes(ref, sem):
        pltpu.make_async_copy(ref, ref, sem).wait()

    def head_norm(block):
        return (block * row_scale(block)).astype(BF16)

    def make_queries(layer):
        hidden = hid[...]
        normed_tgt = (hidden * row_scale(hidden) * tg_v[layer : layer + 1, :]).astype(BF16)
        for head in range(heads):
            cols = slice(head * HEAD_DIM, (head + 1) * HEAD_DIM)
            block = jnp.dot(normed_tgt, wq_v[layer, :, cols], preferred_element_type=F32)
            q_all[layer, head, me_s] = head_norm(block)
            if layer > 0:
                send_queries(layer, head)

    def send_queries(layer, head):
        mine = q_all.at[layer, head, me_s]

        def go(step):
            remote(mine, mine, q_sems, (layer, head), {"sp": sp_peer(step)}).start()

        each(n_sp - 1, go)

    def make_source(layer):
        rows_in = normed[layer]
        big[layer, 1].wait()
        for head in range(heads):
            cols = slice(head * HEAD_DIM, (head + 1) * HEAD_DIM)
            block = jnp.dot(rows_in, wk_v[layer, :, cols], preferred_element_type=F32)
            keys[layer, head] = head_norm(block)
        big[layer, 2].wait()
        for head in range(heads):
            cols = slice(head * HEAD_DIM, (head + 1) * HEAD_DIM)
            block = jnp.dot(rows_in, wv_v[layer, :, cols], preferred_element_type=F32)
            vals[layer, head] = block.astype(BF16)

    chunk = math.gcd(n_sp, 8)
    count = chunk * pad

    def attend(layer, head):
        def one(step):
            first = step * chunk
            queries = q_all[layer, head, pl.ds(first, chunk)].astype(F32)
            scores = lax.dot_general(
                queries.reshape(count, HEAD_DIM).astype(BF16),
                keys[layer, head],
                (((1,), (1,)), ((), ())),
                preferred_element_type=F32,
            )
            weights = jnp.exp(scale_s[layer, head] * (scores / root - root))
            denom = jnp.sum(weights, axis=1, keepdims=True)
            numer = jnp.dot(weights.astype(BF16), vals[layer, head], preferred_element_type=F32)
            high = denom.astype(BF16).astype(F32).reshape(chunk, pad, 1)
            low = denom.reshape(chunk, pad, 1) - high
            lane = lax.broadcasted_iota(jnp.int32, (chunk, pad, HEAD_DIM), 2)
            row = lax.broadcasted_iota(jnp.int32, (chunk, pad, HEAD_DIM), 1)
            spread = jnp.where(lane == row, high, jnp.where(lane == row + pad, low, 0.0))
            packed = jnp.sum(spread, axis=1, keepdims=True)
            block = jnp.where(row == rows, packed, numer.reshape(chunk, pad, HEAD_DIM))
            num_send[layer, head, pl.ds(first, chunk)] = block.astype(BF16)

        each(n_sp // chunk, one)

    def send_numerators(layer, head):
        def go(step):
            peer = sp_peer(step)
            remote(
                num_send.at[layer, head, peer],
                num_recv.at[layer, head, me_s],
                n_sems,
                (layer, head),
                {"sp": peer},
            ).start()

        each(n_sp - 1, go)
        num_recv[layer, head, me_s] = num_send[layer, head, me_s]

    def finish_attention(layer):
        pieces = []
        lane = lax.broadcasted_iota(jnp.int32, (pad, HEAD_DIM), 1)
        row = lax.broadcasted_iota(jnp.int32, (pad, HEAD_DIM), 0)
        mine = (lane == row) | (lane == row + pad)
        for head in range(heads):
            wait_bytes(num_recv.at[layer, head, pl.ds(0, n_sp - 1)], n_sems[1].at[layer, head])
            total = jnp.sum(num_recv[layer, head].astype(F32), axis=0)
            packed = jnp.broadcast_to(total[rows : rows + 1, :], total.shape)
            denom = jnp.sum(jnp.where(mine, packed, 0.0), axis=1, keepdims=True)
            pieces.append((total / denom).astype(BF16))
        return jnp.concatenate(pieces, axis=1)

    def send_shares(layer, attended):
        for part in range(parts):
            cols = slice(part * part_width, (part + 1) * part_width)
            share = jnp.dot(attended, wo_v[layer, :, cols], preferred_element_type=F32)
            shares[layer, part, me_t] = share.astype(BF16)
            mine = shares.at[layer, part, me_t]

            def go(step, mine=mine, part=part):
                remote(mine, mine, s_sems, (layer, part), {"tp": tp_peer(step)}).start()

            each(n_tp - 1, go)

    def add_branch(layer):
        for part in range(parts):
            cols = slice(part * part_width, (part + 1) * part_width)
            wait_bytes(shares.at[layer, part, pl.ds(0, n_tp - 1)], s_sems[1].at[layer, part])
            branch = jnp.sum(shares[layer, part].astype(F32), axis=0)
            total = hid[0:rows, cols] + branch[0:rows, :]
            hid[0:rows, cols] = total.astype(BF16).astype(F32)

    small[0].wait()
    small[1].wait()
    hid[...] = jnp.zeros_like(hid)
    hid[0:rows, :] = tgt_v[...].astype(F32)
    big[0, 0].wait()
    make_queries(0)
    for layer in range(layers):
        for kind in (1, 2, 3, 0):
            if (layer, kind) not in ((0, 0), (0, 1), (0, 2)):
                big[layer, kind].start()
    pl.semaphore_wait(barrier, n_sp - 1 + n_tp - 1)
    for head in range(heads):
        send_queries(0, head)

    small[2].wait()
    small[4].wait()
    step_rows = math.gcd(src_rows, 16)

    def norm_source(layer):
        def norm_rows(index, carry):
            at = pl.ds(pl.multiple_of(index * step_rows, step_rows), step_rows)
            block = src_v[at, :].astype(F32)
            block = block * row_scale(block) * sg_v[layer : layer + 1, :]
            normed[layer, at, :] = block.astype(BF16)
            return carry

        lax.fori_loop(0, src_rows // step_rows, norm_rows, 0, unroll=4)

    norm_source(0)
    small[3].wait()
    make_source(0)

    for layer in range(layers):
        if layer > 0:
            big[layer, 0].wait()
            make_queries(layer)
        for head in range(heads):
            wait_bytes(q_all.at[layer, head, pl.ds(0, n_sp - 1)], q_sems[1].at[layer, head])
            attend(layer, head)
            send_numerators(layer, head)
        if layer + 1 < layers:
            norm_source(layer + 1)
            make_source(layer + 1)
        big[layer, 3].wait()
        send_shares(layer, finish_attention(layer))
        add_branch(layer)

    out_v[...] = hid[0:rows, :].astype(BF16)
    final = pltpu.make_async_copy(out_v, out, load_sem.at[5])
    final.start()
    for layer in range(layers):
        for head in range(heads):
            wait_bytes(q_all.at[layer, head, pl.ds(0, n_sp - 1)], q_sems[0].at[layer, head])
            wait_bytes(num_recv.at[layer, head, pl.ds(0, n_sp - 1)], n_sems[0].at[layer, head])
        for part in range(parts):
            wait_bytes(shares.at[layer, part, pl.ds(0, n_tp - 1)], s_sems[0].at[layer, part])
    final.wait()


def solution(mesh):
    n_sp, n_tp = mesh.shape["sp"], mesh.shape["tp"]
    placed = (
        P("sp", None),
        P("sp", None),
        P(),
        P(),
        P(None, None, "tp"),
        P(None, None, "tp"),
        P(None, None, "tp"),
        P(None, "tp", None),
        P(None, "tp"),
    )

    def body(*args):
        target, source, tgt_gain, src_gain, w_query, w_key, w_value, w_out, score_scale = args
        layers, model, width = w_query.shape
        rows = target.shape[0]
        src_rows = source.shape[0]
        heads = width // HEAD_DIM
        pad = (rows // SUBLANES + 1) * SUBLANES
        anywhere = pl.BlockSpec(memory_space=pl.ANY)
        return pl.pallas_call(
            functools.partial(kernel, n_sp, n_tp),
            out_shape=jax.ShapeDtypeStruct(target.shape, BF16),
            in_specs=[anywhere] * len(args),
            out_specs=anywhere,
            scratch_shapes=[
                pltpu.VMEM(target.shape, BF16),
                pltpu.VMEM(source.shape, BF16),
                pltpu.VMEM(tgt_gain.shape, F32),
                pltpu.VMEM(src_gain.shape, F32),
                pltpu.VMEM(w_query.shape, BF16),
                pltpu.VMEM(w_key.shape, BF16),
                pltpu.VMEM(w_value.shape, BF16),
                pltpu.VMEM(w_out.shape, BF16),
                pltpu.SMEM(score_scale.shape, F32),
                pltpu.VMEM(target.shape, BF16),
                pltpu.VMEM((pad, model), F32),
                pltpu.VMEM((layers, src_rows, model), BF16),
                pltpu.VMEM((layers, heads, src_rows, HEAD_DIM), BF16),
                pltpu.VMEM((layers, heads, src_rows, HEAD_DIM), BF16),
                pltpu.VMEM((layers, heads, n_sp, pad, HEAD_DIM), BF16),
                pltpu.VMEM((layers, heads, n_sp, pad, HEAD_DIM), BF16),
                pltpu.VMEM((layers, heads, n_sp, pad, HEAD_DIM), BF16),
                pltpu.VMEM((layers, PARTS, n_tp, pad, model // PARTS), BF16),
                pltpu.SemaphoreType.DMA((6,)),
                pltpu.SemaphoreType.DMA((layers, 4)),
                *[pltpu.SemaphoreType.DMA((layers, heads))] * 4,
                *[pltpu.SemaphoreType.DMA((layers, PARTS))] * 2,
            ],
            compiler_params=pltpu.CompilerParams(
                collective_id=0, has_side_effects=True, vmem_limit_bytes=60 * 1024 * 1024
            ),
        )(*args)

    return jax.shard_map(
        body, mesh=mesh, in_specs=placed, out_specs=P("sp", None), check_vma=False
    )
```

```python
import functools
import math

import jax
import jax.numpy as jnp
from jax import lax
from jax.experimental import pallas as pl
from jax.experimental.pallas import tpu as pltpu
from jax.sharding import PartitionSpec as P

HEAD_DIM = 256
EPS = 1e-06
PARTS = 2
SUBLANES = 8
MESH = pl.DeviceIdType.MESH
BF16 = jnp.bfloat16
F32 = jnp.float32


def row_scale(values):
    return lax.rsqrt(jnp.mean(values * values, axis=-1, keepdims=True) + EPS)


def each(count, step):
    if count <= 8:
        for index in range(count):
            step(index)
    else:

        def turn(index, carry):
            step(index)
            return carry

        lax.fori_loop(0, count, turn, 0)


def kernel(
    n_sp,
    n_tp,
    target,
    source,
    tgt_gain,
    src_gain,
    w_query,
    w_key,
    w_value,
    w_out,
    score_scale,
    out_hid,
    out_shares,
    tgt_v,
    src_v,
    tg_v,
    sg_v,
    wq_v,
    wk_v,
    wv_v,
    wo_v,
    scale_s,
    hid,
    normed,
    keys,
    vals,
    q_all,
    num_send,
    num_recv,
    shares,
    load_sem,
    keep_sem,
    w_sem,
    *sems,
):
    q_sems, n_sems, s_sems = sems[0:2], sems[2:4], sems[4:6]
    parts, part_width = shares.shape[1], shares.shape[4]
    layers = w_query.shape[0]
    rows = target.shape[0]
    pad = hid.shape[0]
    width = w_query.shape[2]
    heads = width // HEAD_DIM
    src_rows = source.shape[0]
    root = math.sqrt(HEAD_DIM)
    me_s = lax.axis_index("sp")
    me_t = lax.axis_index("tp")

    def peer_of(me, step, size):
        if size & (size - 1):
            return lax.rem(me + step + 1, size)
        distance = size - 1 - step
        peer = me
        bit = 1
        while bit < size:
            here = lax.rem(me // bit, 2)
            flip = (distance // bit) % 2
            peer = peer + flip * bit * (1 - 2 * here)
            bit *= 2
        return peer

    def sp_peer(step):
        return peer_of(me_s, step, n_sp)

    def tp_peer(step):
        return peer_of(me_t, step, n_tp)

    small = [
        pltpu.make_async_copy(target, tgt_v, load_sem.at[0]),
        pltpu.make_async_copy(tgt_gain, tg_v, load_sem.at[1]),
        pltpu.make_async_copy(src_gain, sg_v, load_sem.at[2]),
        pltpu.make_async_copy(score_scale, scale_s, load_sem.at[3]),
        pltpu.make_async_copy(source, src_v, load_sem.at[4]),
    ]
    big = {}
    for layer in range(layers):
        for kind, (hbm, vmem) in enumerate(
            ((w_query, wq_v), (w_key, wk_v), (w_value, wv_v), (w_out, wo_v))
        ):
            big[layer, kind] = pltpu.make_async_copy(
                hbm.at[layer], vmem.at[layer], w_sem.at[layer, kind]
            )
    barrier = pltpu.get_barrier_semaphore()

    def greet_sp(step):
        pl.semaphore_signal(
            barrier, inc=1, device_id={"sp": sp_peer(step)}, device_id_type=MESH
        )

    def greet_tp(step):
        pl.semaphore_signal(
            barrier, inc=1, device_id={"tp": tp_peer(step)}, device_id_type=MESH
        )

    each(n_sp - 1, greet_sp)
    each(n_tp - 1, greet_tp)

    for index in (0, 1):
        small[index].start()
    big[0, 0].start()
    for index in (4, 2, 3):
        small[index].start()
    big[0, 1].start()
    big[0, 2].start()

    def remote(src, dst, sems, at, target_id):
        return pltpu.make_async_remote_copy(
            src_ref=src,
            dst_ref=dst,
            send_sem=sems[0].at[at],
            recv_sem=sems[1].at[at],
            device_id=target_id,
            device_id_type=MESH,
        )

    def wait_bytes(ref, sem):
        pltpu.make_async_copy(ref, ref, sem).wait()

    def head_norm(block):
        return (block * row_scale(block)).astype(BF16)

    def make_queries(layer):
        hidden = hid[...]
        scale = row_scale(hidden)
        gained = (hidden * tg_v[layer : layer + 1, :]).astype(BF16)
        for head in range(heads):
            cols = slice(head * HEAD_DIM, (head + 1) * HEAD_DIM)
            block = jnp.dot(gained, wq_v[layer, :, cols], preferred_element_type=F32)
            q_all[layer, me_s, head] = head_norm(block * scale)

    def send_queries(layer):
        mine = q_all.at[layer, me_s]

        def go(step):
            remote(mine, mine, q_sems, layer, {"sp": sp_peer(step)}).start()

        each(n_sp - 1, go)

    def make_source(layer):
        rows_in = normed[layer]
        big[layer, 1].wait()
        for head in range(heads):
            cols = slice(head * HEAD_DIM, (head + 1) * HEAD_DIM)
            block = jnp.dot(rows_in, wk_v[layer, :, cols], preferred_element_type=F32)
            keys[layer, head] = head_norm(block)
        big[layer, 2].wait()
        for head in range(heads):
            cols = slice(head * HEAD_DIM, (head + 1) * HEAD_DIM)
            block = jnp.dot(rows_in, wv_v[layer, :, cols], preferred_element_type=F32)
            vals[layer, head] = block.astype(BF16)

    chunk = math.gcd(n_sp, 8)
    count = chunk * pad

    def attend(layer):
        def one(step):
            first = step * chunk
            lane = lax.broadcasted_iota(jnp.int32, (chunk, pad, HEAD_DIM), 2)
            row = lax.broadcasted_iota(jnp.int32, (chunk, pad, HEAD_DIM), 1)
            for head in range(heads):
                queries = q_all[layer, pl.ds(first, chunk), head].astype(F32)
                scores = lax.dot_general(
                    queries.reshape(count, HEAD_DIM).astype(BF16),
                    keys[layer, head],
                    (((1,), (1,)), ((), ())),
                    preferred_element_type=F32,
                )
                weights = jnp.exp(scale_s[layer, head] * (scores / root - root))
                denom = jnp.sum(weights, axis=1, keepdims=True)
                numer = jnp.dot(
                    weights.astype(BF16), vals[layer, head], preferred_element_type=F32
                )
                high = denom.astype(BF16).astype(F32).reshape(chunk, pad, 1)
                low = denom.reshape(chunk, pad, 1) - high
                spread = jnp.where(lane == row, high, jnp.where(lane == row + pad, low, 0.0))
                packed = jnp.sum(spread, axis=1, keepdims=True)
                block = jnp.where(row == rows, packed, numer.reshape(chunk, pad, HEAD_DIM))
                num_send[layer, pl.ds(first, chunk), head] = block.astype(BF16)

        each(n_sp // chunk, one)

    def send_numerators(layer):
        def go(step):
            peer = sp_peer(step)
            remote(
                num_send.at[layer, peer],
                num_recv.at[layer, me_s],
                n_sems,
                layer,
                {"sp": peer},
            ).start()

        each(n_sp - 1, go)
        num_recv[layer, me_s] = num_send[layer, me_s]

    def finish_attention(layer):
        pieces = []
        lane = lax.broadcasted_iota(jnp.int32, (pad, HEAD_DIM), 1)
        row = lax.broadcasted_iota(jnp.int32, (pad, HEAD_DIM), 0)
        mine = (lane == row) | (lane == row + pad)
        wait_bytes(num_recv.at[layer, pl.ds(0, n_sp - 1)], n_sems[1].at[layer])
        for head in range(heads):
            total = jnp.sum(num_recv[layer, :, head].astype(F32), axis=0)
            packed = jnp.broadcast_to(total[rows : rows + 1, :], total.shape)
            denom = jnp.sum(jnp.where(mine, packed, 0.0), axis=1, keepdims=True)
            pieces.append((total / denom).astype(BF16))
        return jnp.concatenate(pieces, axis=1)

    def send_shares(layer, attended):
        for part in range(parts):
            cols = slice(part * part_width, (part + 1) * part_width)
            share = jnp.dot(attended, wo_v[layer, :, cols], preferred_element_type=F32)
            shares[layer, part, me_t] = share.astype(BF16)
            mine = shares.at[layer, part, me_t]
            there = mine if layer + 1 < layers else out_shares.at[me_t, :, cols]

            def go(step, mine=mine, there=there, part=part):
                remote(mine, there, s_sems, (layer, part), {"tp": tp_peer(step)}).start()

            each(n_tp - 1, go)
            if layer + 1 == layers:
                pltpu.make_async_copy(mine, there, keep_sem.at[part]).start()

    def add_branch(layer):
        for part in range(parts):
            cols = slice(part * part_width, (part + 1) * part_width)
            wait_bytes(shares.at[layer, part, pl.ds(0, n_tp - 1)], s_sems[1].at[layer, part])
            branch = jnp.sum(shares[layer, part].astype(F32), axis=0)
            total = hid[0:rows, cols] + branch[0:rows, :]
            hid[0:rows, cols] = total.astype(BF16).astype(F32)

    small[0].wait()
    small[1].wait()
    hid[...] = jnp.zeros_like(hid)
    hid[0:rows, :] = tgt_v[...].astype(F32)
    big[0, 0].wait()
    make_queries(0)
    for layer in range(layers):
        for kind in (1, 2, 3, 0):
            if (layer, kind) not in ((0, 0), (0, 1), (0, 2)):
                big[layer, kind].start()
    pl.semaphore_wait(barrier, n_sp - 1 + n_tp - 1)
    send_queries(0)

    small[2].wait()
    small[4].wait()
    step_rows = math.gcd(src_rows, 16)

    def norm_source(layer):
        def norm_rows(index, carry):
            at = pl.ds(pl.multiple_of(index * step_rows, step_rows), step_rows)
            block = src_v[at, :].astype(F32)
            block = block * row_scale(block) * sg_v[layer : layer + 1, :]
            normed[layer, at, :] = block.astype(BF16)
            return carry

        lax.fori_loop(0, src_rows // step_rows, norm_rows, 0, unroll=4)

    norm_source(0)
    small[3].wait()
    make_source(0)

    for layer in range(layers):
        if layer > 0:
            big[layer, 0].wait()
            make_queries(layer)
            send_queries(layer)
        if layer + 1 == layers:
            tgt_v[...] = hid[0:rows, :].astype(BF16)
            keep_hidden = pltpu.make_async_copy(tgt_v, out_hid, load_sem.at[0])
            keep_hidden.start()
        wait_bytes(q_all.at[layer, pl.ds(0, n_sp - 1)], q_sems[1].at[layer])
        attend(layer)
        send_numerators(layer)
        if layer + 1 < layers:
            norm_source(layer + 1)
            make_source(layer + 1)
        big[layer, 3].wait()
        send_shares(layer, finish_attention(layer))
        if layer + 1 < layers:
            add_branch(layer)

    for part in range(parts):
        cols = slice(part * part_width, (part + 1) * part_width)
        arrived = out_shares.at[pl.ds(0, n_tp - 1), :, cols]
        wait_bytes(arrived, s_sems[1].at[layers - 1, part])
        pltpu.make_async_copy(
            shares.at[layers - 1, part, me_t], out_shares.at[me_t, :, cols], keep_sem.at[part]
        ).wait()
    keep_hidden.wait()
    for layer in range(layers):
        wait_bytes(q_all.at[layer, pl.ds(0, n_sp - 1)], q_sems[0].at[layer])
        wait_bytes(num_recv.at[layer, pl.ds(0, n_sp - 1)], n_sems[0].at[layer])
        for part in range(parts):
            wait_bytes(shares.at[layer, part, pl.ds(0, n_tp - 1)], s_sems[0].at[layer, part])


def solution(mesh):
    n_sp, n_tp = mesh.shape["sp"], mesh.shape["tp"]
    placed = (
        P("sp", None),
        P("sp", None),
        P(),
        P(),
        P(None, None, "tp"),
        P(None, None, "tp"),
        P(None, None, "tp"),
        P(None, "tp", None),
        P(None, "tp"),
    )

    def body(*args):
        target, source, tgt_gain, src_gain, w_query, w_key, w_value, w_out, score_scale = args
        layers, model, width = w_query.shape
        rows = target.shape[0]
        src_rows = source.shape[0]
        heads = width // HEAD_DIM
        pad = (rows // SUBLANES + 1) * SUBLANES
        anywhere = pl.BlockSpec(memory_space=pltpu.HBM)
        hidden, last_shares = pl.pallas_call(
            functools.partial(kernel, n_sp, n_tp),
            out_shape=(
                jax.ShapeDtypeStruct(target.shape, BF16),
                jax.ShapeDtypeStruct((n_tp, pad, model), BF16),
            ),
            in_specs=[anywhere] * len(args),
            out_specs=(anywhere, anywhere),
            scratch_shapes=[
                pltpu.VMEM(target.shape, BF16),
                pltpu.VMEM(source.shape, BF16),
                pltpu.VMEM(tgt_gain.shape, F32),
                pltpu.VMEM(src_gain.shape, F32),
                pltpu.VMEM(w_query.shape, BF16),
                pltpu.VMEM(w_key.shape, BF16),
                pltpu.VMEM(w_value.shape, BF16),
                pltpu.VMEM(w_out.shape, BF16),
                pltpu.SMEM(score_scale.shape, F32),
                pltpu.VMEM((pad, model), F32),
                pltpu.VMEM((layers, src_rows, model), BF16),
                pltpu.VMEM((layers, heads, src_rows, HEAD_DIM), BF16),
                pltpu.VMEM((layers, heads, src_rows, HEAD_DIM), BF16),
                pltpu.VMEM((layers, n_sp, heads, pad, HEAD_DIM), BF16),
                pltpu.VMEM((layers, n_sp, heads, pad, HEAD_DIM), BF16),
                pltpu.VMEM((layers, n_sp, heads, pad, HEAD_DIM), BF16),
                pltpu.VMEM((layers, PARTS, n_tp, pad, model // PARTS), BF16),
                pltpu.SemaphoreType.DMA((5,)),
                pltpu.SemaphoreType.DMA((PARTS,)),
                pltpu.SemaphoreType.DMA((layers, 4)),
                *[pltpu.SemaphoreType.DMA((layers,))] * 4,
                *[pltpu.SemaphoreType.DMA((layers, PARTS))] * 2,
            ],
            compiler_params=pltpu.CompilerParams(
                collective_id=0, has_side_effects=True, vmem_limit_bytes=60 * 1024 * 1024
            ),
        )(*args)
        branch = last_shares[0, :rows].astype(F32)
        for group in range(1, n_tp):
            branch = branch + last_shares[group, :rows].astype(F32)
        return (hidden.astype(F32) + branch).astype(BF16)

    return jax.shard_map(
        body, mesh=mesh, in_specs=placed, out_specs=P("sp", None), check_vma=False
    )
```
